32 devices in a mesh: grp: 2 (over y), sp: 4 (over z), tp: 4 (over x, core).
Axes of the slice: x: 2, y: 2, z: 4, core: 2. Of those that a mesh axis runs over, the one named last changes fastest.
Arguments:
- queries: bfloat16 [1024, 2048], P(('grp', 'sp'), 'tp'), parts along dimension 0, may hold values from -8 to 8
- keys: bfloat16 [1024, 1024], P(('grp', 'sp'), 'tp'), parts along dimension 0, may hold values from -6 to 6
- values: bfloat16 [1024, 1024], P(('grp', 'sp'), 'tp'), parts along dimension 0, may hold values from -6 to 6
- head_bias: float32 [16], P('tp'), may hold values from -15 to -5
- documents: int32 [1024], P(('grp', 'sp')), parts along dimension 0, may hold values from 0 to 2, never falling along the last dimension, each value on 1 to 384 neighbouring positions
- w_out: bfloat16 [2048, 2048], P('tp'), may hold values from -0.125 to 0.125
- resid: bfloat16 [1024, 2048], P(('grp', 'sp', 'tp')), parts along dimension 0, may hold values from -6 to 6
- norm_gain: float32 [2048], replicated, may hold values from 0.1 to 1.9
- expert_ids: int32 [1024, 2], P(('grp', 'sp', 'tp')), parts along dimension 0, may hold values from 0 to 3, all different within a row; in each aligned block of 32 rows (0 to 31, 32 to 63, ...) at most 32 rows name the same one
- expert_gates: float32 [1024, 2], P(('grp', 'sp', 'tp')), parts along dimension 0, may hold values from 0.1 to 0.9
- w_gate: bfloat16 [4, 2048, 3072], P('sp', None, 'tp'), may hold values from -0.125 to 0.125
- w_up: bfloat16 [4, 2048, 3072], P('sp', None, 'tp'), may hold values from -0.125 to 0.125
- w_down: bfloat16 [4, 3072, 2048], P('sp', 'tp'), may hold values from -0.109375 to 0.109375
Outputs:
- layer_out: bfloat16 [1024, 2048], P(('grp', 'sp', 'tp')), parts along dimension 0
The draws below stay inside these ranges and needn't reach their ends.
There are 2 independent parts, one for each index of `grp`. The reference program is written for one: setup_inputs(seed, part) draws one part's arguments, and reference() takes and returns one part's arrays. A program takes and returns all parts, laid end to end along the dimension named above; an argument that names none is the same for every part. Nothing has to cross between parts.
Inputs may be any that keep to these rules, and one draw needn't show every extreme that they name: Document numbers never fall along the sequence; each of the 3 documents holds at least one position and the longest exactly 384 positions. `expert_ids`: each position names 2 different experts. Among the 32 positions of one device (aligned blocks of 32 rows) no expert is named more than 32 times, and in some block some expert exactly 32 times.
All inputs are finite; a program needn't handle non-finite values.
Results may differ from the reference program's by a relative error of at most 0.012.
Values may be sent and summed in bfloat16 or wider, within the bound.
No kernel may reach another device: no remote copies, remote signals or barrier semaphores. Data moves between devices by JAX's collectives and lax.ppermute only.
A program may use at most 64 MiB of HBM per device.

```python
import math
import jax
import jax.numpy as jnp
import numpy as np
from jax import lax

D = 2048
HEADS = 16
KV_HEADS = 8
DH = 128
FF = 3072
TOPK = 2
DOCS = 3
SEQ = 512
ROWS = 32
EXPERTS = 4
CAP = 32
N_SP = 4
N_TP = 4


def draw_head_bias(key, part):
    return jax.random.uniform(key, (HEADS,), jnp.float32, -14.0, -5.0)


def shard_levels(own_key, dims, split, least, largest):
    gain, own = 1.0, jax.random.fold_in(own_key, 6)
    for axis_at, parts in split:
        steps = jnp.exp(jax.random.uniform(jax.random.fold_in(own, axis_at), (parts,), jnp.float32, least / len(split), largest / len(split)))
        gain = gain * jnp.repeat(steps, dims[axis_at] // parts).reshape([-1 if axis == axis_at else 1 for axis in range(len(dims))])
    return gain


def split_up(amount, total, reach, lean):
    loads = [(1 << 20) // math.isqrt(rank ** lean) + 1 for rank in range(2, amount + 1)]
    spare, holding = total - reach - (amount - 1), [1] * (amount - 1)
    while spare > 0:
        free = [i for i in range(amount - 1) if holding[i] < reach]
        whole, remaining = sum([loads[i] for i in free]), spare
        for i in free:
            extra = min(reach - holding[i], max(1, remaining * loads[i] // whole), spare)
            holding[i] = holding[i] + extra
            spare = spare - extra
    return np.array([reach] + holding)


def ragged_sizes(rng, count, total, reach, slope):
    if count == 2:
        one = jax.random.randint(rng, (), max(1, total - reach), min(reach, total - 1) + 1)
        return jnp.stack([one, total - one])
    sizes = jnp.asarray(split_up(count, total, reach, slope), jnp.int32)
    couples = (count - 1) // 2
    giver, taker = sizes[1:1 + 2 * couples:2], sizes[2:2 + 2 * couples:2]
    slack = jnp.minimum(giver - 1, reach - taker)
    shifted = jax.random.randint(jax.random.fold_in(rng, 1), (couples,), 0, 1 << 20) % (slack + 1)
    sizes = sizes.at[1:1 + 2 * couples:2].set(giver - shifted).at[2:2 + 2 * couples:2].set(taker + shifted)
    return sizes[jax.random.permutation(jax.random.fold_in(rng, 2), count)]


def assign_block(own_key, own, number, rows, number_of, top, most, slope):
    order = jax.random.permutation(own_key, number_of)
    packed, common = shares(number_of, rows * top, most, slope, True), shares(number_of, rows * top, most, slope, False)
    places = jnp.arange(number_of)

    def named(tallies, offset_by):
        used = int((tallies > 0).sum())
        fixed = max(1, used // 4)
        shifted = fixed + (places - fixed + offset_by * (used - fixed)) % max(1, number_of - fixed)
        return jnp.zeros((number_of,), jnp.int32).at[order[jnp.where(places < fixed, places, shifted)]].set(jnp.asarray(tallies, jnp.int32))

    tallies = jnp.where(number % 4 == 0, named(packed, number // 4), named(common, number - number // 4 - 1))
    mixed = jax.random.permutation(jax.random.fold_in(own, 3), number_of)
    donor, taker = mixed[0:number_of // 2 * 2:2], mixed[1:number_of // 2 * 2:2]
    room = jnp.minimum(tallies[donor] - 1, most - tallies[taker]) // 2
    room = jnp.where((donor == order[0]) | (taker == order[0]) | (tallies[taker] == 0), 0, jnp.maximum(room, 0))
    shifted = jax.random.randint(jax.random.fold_in(own, 4), (number_of // 2,), 0, 1 << 20) % (room + 1)
    tallies = tallies.at[donor].add(-shifted).at[taker].add(shifted)
    labels = jnp.searchsorted(jnp.cumsum(tallies), jnp.arange(rows * top), side="right").astype(jnp.int32)
    table = labels.reshape(top, rows).T
    table = table[jax.random.permutation(jax.random.fold_in(own, 1), rows)]
    offset_by = jax.random.randint(jax.random.fold_in(own, 2), (rows, 1), 0, top)
    return jnp.take_along_axis(table, (jnp.arange(top)[None, :] + offset_by) % top, axis=1)


def shares(amount, total, reach, skew, full):
    loads = [(1 << 20) // math.isqrt(grade ** skew) + 1 for grade in range(1, amount + 1)]
    largest = reach if full else min(reach, max(-(-total // amount), total * loads[0] // sum(loads)))
    least = 1 if total - largest >= amount - 1 else 0
    given, rest = [largest] + [least] * (amount - 1), total - largest - least * (amount - 1)
    while rest > 0:
        candidates = [i for i in range(1, amount) if given[i] < largest] or [i for i in range(1, amount) if given[i] < reach]
        whole, budget = sum([loads[i] for i in candidates]), rest
        for i in candidates:
            extra = min(reach - given[i], max(1, budget * loads[i] // whole), rest)
            given[i] = given[i] + extra
            rest = rest - extra
    return np.array(given)


def centred(own_key, shape, width, most, split=(), kind=jnp.bfloat16):
    result = jax.random.normal(own_key, shape, jnp.float32) * width
    if len(split) > 0:
        result = shard_levels(own_key, shape, split, -0.22, 0.18) * result
    return jnp.clip(result, min=-most, max=most).astype(kind)


def setup_inputs(seed: int = 0, part: int = 0) -> dict:
    key_list = jax.random.split(jax.random.key(seed), 14)
    own_keys = jax.random.split(jax.random.fold_in(key_list[13], part), 14)
    queries = centred(own_keys[0], (SEQ, HEADS * DH), 2.0, 8.0, ((0, 4), (1, 4)))
    keys = centred(own_keys[1], (SEQ, KV_HEADS * DH), 1.0, 6.0, ((0, 4), (1, 4)))
    values = centred(own_keys[2], (SEQ, KV_HEADS * DH), 1.0, 6.0, ((0, 4), (1, 4)))
    head_bias = draw_head_bias(jax.random.fold_in(key_list[13], 71), part)
    documents = jnp.searchsorted(jnp.cumsum(ragged_sizes(own_keys[4], DOCS, SEQ, 3 * SEQ // 4, 0)), jnp.arange(SEQ), side="right").astype(jnp.int32)
    w_out = centred(key_list[5], (HEADS * DH, D), (HEADS * DH) ** -0.5, 0.125, ((0, 4),))
    resid = centred(own_keys[6], (SEQ, D), 1.0, 6.0, ((0, 16),))
    norm_gain = jnp.clip(1.0 + 0.18 * jax.random.normal(key_list[7], (D,), jnp.float32), 0.1, 1.9)
    expert_ids_keys = jax.random.split(jax.random.fold_in(own_keys[8], 1), SEQ // ROWS)
    expert_ids_turns = jax.random.permutation(jax.random.fold_in(own_keys[8], 3), SEQ // ROWS)
    expert_ids = jax.vmap(lambda own, number: assign_block(jax.random.fold_in(own_keys[8], 2), own, number, ROWS, EXPERTS, TOPK, CAP, 1))(expert_ids_keys, expert_ids_turns).reshape((SEQ, TOPK))
    expert_gates = jnp.clip(0.1 + 0.79999997 * jax.random.uniform(own_keys[9], (SEQ, TOPK), jnp.float32) ** shard_levels(own_keys[9], (SEQ, TOPK), ((0, 16),), -0.2, 0.2), 0.1, 0.9)
    w_gate = centred(key_list[10], (EXPERTS, D, FF), D ** -0.5, 0.125, ((0, 4), (2, 4)))
    w_up = centred(key_list[11], (EXPERTS, D, FF), D ** -0.5, 0.125, ((0, 4), (2, 4)))
    w_down = centred(key_list[12], (EXPERTS, FF, D), FF ** -0.5, 0.109375, ((0, 4), (1, 4)))
    return {"queries": queries, "keys": keys, "values": values, "head_bias": head_bias, "documents": documents, "w_out": w_out, "resid": resid, "norm_gain": norm_gain, "expert_ids": expert_ids, "expert_gates": expert_gates, "w_gate": w_gate, "w_up": w_up, "w_down": w_down}


def rounded(array):
    return lax.optimization_barrier(array.astype(jnp.bfloat16)).astype(jnp.float32)

def reference(queries, keys, values, head_bias, documents, w_out, resid, norm_gain, expert_ids, expert_gates, w_gate, w_up, w_down):
    highest = lax.Precision.HIGHEST
    group_size = HEADS // KV_HEADS
    scale_factor = DH ** (-0.5)
    query_all = queries.astype(jnp.float32).reshape(SEQ, KV_HEADS, group_size, DH)
    key_all = keys.astype(jnp.float32).reshape(SEQ, KV_HEADS, DH)
    value_all = values.astype(jnp.float32).reshape(SEQ, KV_HEADS, DH)
    bias_grid = head_bias.astype(jnp.float32).reshape(KV_HEADS, group_size)
    positions = jnp.arange(SEQ, dtype=jnp.int32)
    block_rows = math.gcd(SEQ, 256)

    def attend_block(block_index):
        first = block_index * block_rows
        query_block = lax.dynamic_slice_in_dim(query_all, first, block_rows, 0)
        query_pos = first + jnp.arange(block_rows, dtype=jnp.int32)
        query_doc = lax.dynamic_slice_in_dim(documents, first, block_rows, 0)
        live = (positions[None, :] < query_pos[:, None]) & (documents[None, :] == query_doc[:, None])
        logits = jnp.einsum('qgrd,sgd->grqs', query_block, key_all, precision=highest) * scale_factor + bias_grid[:, :, None, None]
        keep = jnp.where(live, jax.nn.log_sigmoid(-logits), 0.0)
        after = lax.cumsum(keep, axis=3, reverse=True) - keep
        weight = rounded(jnp.where(live, jnp.exp(jax.nn.log_sigmoid(logits) + after), 0.0))
        mixed_block = jnp.einsum('grqs,sgd->qgrd', weight, value_all, precision=highest)
        return mixed_block.reshape(block_rows, HEADS * DH).astype(jnp.bfloat16)
    mixed = lax.map(attend_block, jnp.arange(SEQ // block_rows, dtype=jnp.int32)).reshape(SEQ, HEADS * DH)
    share = HEADS * DH // N_TP
    partials = jnp.einsum('sjc,jcd->sjd', mixed.astype(jnp.float32).reshape(SEQ, N_TP, share), w_out.astype(jnp.float32).reshape(N_TP, share, D), precision=highest)
    middle = (resid.astype(jnp.float32) + lax.optimization_barrier(jnp.sum(rounded(partials), axis=1))).astype(jnp.bfloat16)
    middle_value = middle.astype(jnp.float32)
    normed = (middle_value * lax.rsqrt(lax.optimization_barrier(jnp.mean(middle_value * middle_value, axis=1, keepdims=True)) + 1e-06) * norm_gain.astype(jnp.float32)).astype(jnp.bfloat16)
    assignments = SEQ * TOPK
    most_rows = N_SP * N_TP * CAP
    flat_ids = expert_ids.reshape(-1)
    hidden_share = FF // N_TP

    def run_expert(expert):
        picks = jnp.nonzero(flat_ids == expert, size=most_rows, fill_value=assignments)[0].astype(jnp.int32)
        source = normed[jnp.minimum(picks, assignments - 1) // TOPK].astype(jnp.float32)
        gate_value = jnp.dot(source, w_gate[expert].astype(jnp.float32), precision=highest)
        up_value = jnp.dot(source, w_up[expert].astype(jnp.float32), precision=highest)
        hidden = rounded(jax.nn.silu(gate_value) * up_value).reshape(most_rows, N_TP, hidden_share)
        partial_out = jnp.einsum('bjf,jfd->bjd', hidden, w_down[expert].astype(jnp.float32).reshape(N_TP, hidden_share, D), precision=highest)
        return (lax.optimization_barrier(jnp.sum(rounded(partial_out), axis=1)).astype(jnp.bfloat16), picks)
    outputs, picks_all = lax.map(run_expert, jnp.arange(EXPERTS, dtype=jnp.int32))
    routed = jnp.zeros((assignments, D), jnp.bfloat16).at[picks_all.reshape(-1)].set(outputs.reshape(-1, D), mode='drop')
    combined = lax.optimization_barrier(jnp.sum(expert_gates.astype(jnp.float32)[:, :, None] * routed.reshape(SEQ, TOPK, D).astype(jnp.float32), axis=1))
    return (middle_value + combined).astype(jnp.bfloat16)
```

```python
import functools

import jax
import jax.numpy as jnp
from jax import lax
from jax.experimental import pallas as pl
from jax.experimental.pallas import tpu as pltpu
from jax.sharding import PartitionSpec as P

D = 2048
HEADS = 16
KV_HEADS = 8
DH = 128
TOPK = 2
DOC_ROWS = 16
DIRECT_KEYS = 1024
VMEM = pl.BlockSpec(memory_space=pltpu.VMEM)
SMEM = pl.BlockSpec(memory_space=pltpu.SMEM)


def shifted(value, steps, wrap):
    count = lax.axis_size("sp")
    pairs = [(i, (i + steps) % count) for i in range(count) if wrap or 0 <= i + steps < count]
    return lax.ppermute(value, "sp", pairs)


def swapped(value, mask):
    count = lax.axis_size("tp")
    return lax.ppermute(value, "tp", [(i, i ^ mask) for i in range(count)])


def block_terms(q_ref, bias_ref, key_of, value_of, live, carry):
    heads = q_ref.shape[1] // DH
    group = HEADS // KV_HEADS
    rows = q_ref.shape[0]
    parts = []
    for h in range(heads):
        part = lax.dot_general(
            q_ref[:, h * DH : (h + 1) * DH],
            key_of(h // group),
            (((1,), (1,)), ((), ())),
            preferred_element_type=jnp.float32,
        )
        parts.append(part * DH ** (-0.5) + bias_ref[h])
    logits = jnp.concatenate(parts, axis=0)
    live = jnp.concatenate([live] * heads, axis=0)
    soft = jnp.log1p(jnp.exp(-jnp.abs(logits)))
    keep = jnp.where(live, -jnp.maximum(logits, 0.0) - soft, 0.0)
    keys = logits.shape[1]
    later = lax.broadcasted_iota(jnp.int32, (keys, keys), 0) > lax.broadcasted_iota(
        jnp.int32, (keys, keys), 1
    )
    later = later.astype(jnp.float32).astype(jnp.bfloat16)
    high = keep.astype(jnp.bfloat16)
    low = (keep - high.astype(jnp.float32)).astype(jnp.bfloat16)
    after = jnp.dot(high, later, preferred_element_type=jnp.float32) + jnp.dot(
        low, later, preferred_element_type=jnp.float32
    )
    weight = jnp.where(
        live, jnp.exp(jnp.minimum(logits, 0.0) - soft + after + carry), 0.0
    ).astype(jnp.bfloat16)
    mixes = [
        jnp.dot(
            weight[h * rows : (h + 1) * rows], value_of(h // group), preferred_element_type=jnp.float32
        )
        for h in range(heads)
    ]
    return jnp.concatenate(mixes, axis=1), carry + jnp.sum(keep, axis=1, keepdims=True)


def here_kernel(q_ref, k_ref, v_ref, bias_ref, col_ref, row_ref, mix_ref, carry_ref):
    rows = q_ref.shape[0]
    causal = lax.broadcasted_iota(jnp.int32, (rows, rows), 1) < lax.broadcasted_iota(
        jnp.int32, (rows, rows), 0
    )
    live = causal & (col_ref[...] == row_ref[...])
    carry = jnp.zeros((rows * (q_ref.shape[1] // DH), 1), jnp.float32)
    mix, carry = block_terms(
        q_ref,
        bias_ref,
        lambda g: k_ref[:, g * DH : (g + 1) * DH],
        lambda g: v_ref[:, g * DH : (g + 1) * DH],
        live,
        carry,
    )
    mix_ref[...] = mix
    carry_ref[...] = jnp.broadcast_to(carry, carry_ref.shape)


def away_kernel(count, order, place_ref, q_ref, bias_ref, col_ref, mix_ref, carry_ref, w_ref, *refs):
    sent, outs, mixed_ref = refs[:count], refs[count:-1], refs[-1]
    rows = q_ref.shape[0]
    width = q_ref.shape[1] // (HEADS // KV_HEADS)
    mix = mix_ref[...]
    carry = carry_ref[:, 0:1]
    for step, block in enumerate(sent, 1):
        doc_row = block[rows : rows + 1, 0:rows].astype(jnp.float32)
        doc_row = jnp.where(place_ref[0] >= step, doc_row, -1.0)
        live = col_ref[...] == doc_row
        term, carry = block_terms(
            q_ref,
            bias_ref,
            lambda g, block=block: block[0:rows, g * DH : (g + 1) * DH],
            lambda g, block=block: block[0:rows, width + g * DH : width + (g + 1) * DH],
            live,
            carry,
        )
        mix = mix + term
    mixed_ref[...] = mix
    share = rows // len(order)
    for mask, out in zip(order, outs):
        first = pl.multiple_of((place_ref[1] ^ mask) * share, share)
        piece = mixed_ref[pl.ds(first, share), :].astype(jnp.bfloat16)
        out[...] = jnp.dot(piece, w_ref[...], preferred_element_type=jnp.float32).astype(jnp.bfloat16)


def norm_kernel(resid_ref, gain_ref, *refs):
    pieces, middle_ref, normed_ref = refs[:-2], refs[-2], refs[-1]
    total = pieces[0][...].astype(jnp.float32)
    for piece in pieces[1:]:
        total = total + piece[...].astype(jnp.float32)
    middle = (resid_ref[...].astype(jnp.float32) + total).astype(jnp.bfloat16)
    middle_ref[...] = middle
    value = middle.astype(jnp.float32)
    scale = lax.rsqrt(jnp.mean(value * value, axis=1, keepdims=True) + 1e-06)
    normed_ref[...] = (value * scale * gain_ref[...]).astype(jnp.bfloat16)


def cost(flops, nbytes):
    return pl.CostEstimate(flops=flops, bytes_accessed=nbytes, transcendentals=0)


def middle_direct(queries, keys, values, head_bias, documents, w_out, resid, norm_gain):
    rows, width = queries.shape
    kv_width = keys.shape[1]
    sp_count = lax.axis_size("sp")
    tp_count = lax.axis_size("tp")
    doc_real = documents.astype(jnp.bfloat16)
    doc_rows = jnp.zeros((DOC_ROWS, 2 * kv_width), jnp.bfloat16)
    doc_rows = doc_rows.at[0, :rows].set(doc_real)
    packed = jnp.concatenate([jnp.concatenate([keys, values], axis=1), doc_rows], axis=0)
    sent = [shifted(packed, steps, False) for steps in range(1, sp_count)]
    col = documents.astype(jnp.float32).reshape(rows, 1)
    row = documents.astype(jnp.float32).reshape(1, rows)
    heads = width // DH
    mix, carry = pl.pallas_call(
        here_kernel,
        out_shape=(
            jax.ShapeDtypeStruct((rows, width), jnp.float32),
            jax.ShapeDtypeStruct((rows * heads, DH), jnp.float32),
        ),
        in_specs=[VMEM, VMEM, VMEM, SMEM, VMEM, VMEM],
        out_specs=(VMEM, VMEM),
        cost_estimate=cost(6 * 10**9, 10**6),
        name="attend_here",
    )(queries, keys, values, head_bias, col, row)
    place = jnp.stack([lax.axis_index("sp"), lax.axis_index("tp")]).astype(jnp.int32)
    order = list(range(tp_count))
    share = rows // tp_count
    pieces = pl.pallas_call(
        functools.partial(away_kernel, sp_count - 1, order),
        out_shape=[jax.ShapeDtypeStruct((share, D), jnp.bfloat16)] * tp_count,
        in_specs=[SMEM, VMEM, SMEM, VMEM, VMEM, VMEM, VMEM] + [VMEM] * (sp_count - 1),
        out_specs=[VMEM] * tp_count,
        scratch_shapes=[pltpu.VMEM((rows, width), jnp.float32)],
        cost_estimate=cost(10 * 10**9, 4 * 10**6),
        name="attend_away",
    )(place, queries, head_bias, col, mix, carry, w_out, *sent)
    arrived = [pieces[0]] + [swapped(pieces[mask], mask) for mask in order[:0:-1]]
    return pl.pallas_call(
        norm_kernel,
        out_shape=[jax.ShapeDtypeStruct((share, D), jnp.bfloat16)] * 2,
        in_specs=[VMEM] * (2 + tp_count),
        out_specs=[VMEM] * 2,
        cost_estimate=cost(10**8, 10**6),
        name="middle_norm",
    )(resid, norm_gain.reshape(1, D), *arrived)


def experts_dense(middle, normed, expert_ids, expert_gates, w_gate, w_up, w_down):
    rows = normed.shape[0]
    sp_count = lax.axis_size("sp")
    tp_count = lax.axis_size("tp")
    masks = [1 << bit for bit in range(tp_count.bit_length() - 1)]
    steps = [0] + [s for pair in zip(range(1, sp_count), range(sp_count - 1, 0, -1)) for s in pair]
    steps = list(dict.fromkeys(steps))
    half = (len(steps) + 1) // 2
    moved = {s: normed if s == 0 else shifted(normed, s, True) for s in steps}
    pieces = {}
    for chunk in (steps[:half], steps[half:]):
        held = jnp.concatenate([moved[s] for s in chunk], axis=0)
        for mask in masks[::-1]:
            held = jnp.concatenate([held, swapped(held, mask)], axis=0)
        gate_value = jnp.dot(held, w_gate[0], preferred_element_type=jnp.float32)
        up_value = jnp.dot(held, w_up[0], preferred_element_type=jnp.float32)
        hidden = (jax.nn.silu(gate_value) * up_value).astype(jnp.bfloat16)
        result = jnp.dot(hidden, w_down[0], preferred_element_type=jnp.float32).astype(jnp.bfloat16)
        for mask in masks:
            kept = result.shape[0] // 2
            result = (
                result[:kept].astype(jnp.float32) + swapped(result[kept:], mask).astype(jnp.float32)
            ).astype(jnp.bfloat16)
        for at, s in enumerate(chunk):
            pieces[s] = result[at * rows : (at + 1) * rows]
    own = lax.axis_index("sp")
    total = middle.astype(jnp.float32)
    combined = jnp.zeros_like(total)
    for s in steps:
        piece = pieces[s] if s == 0 else shifted(pieces[s], -s, True)
        chosen = expert_ids == (own + s) % sp_count
        scale = jnp.sum(jnp.where(chosen, expert_gates, 0.0), axis=1, keepdims=True)
        combined = combined + scale * piece.astype(jnp.float32)
    return (total + combined).astype(jnp.bfloat16)


def passed_along(value, axis, steps):
    count = lax.axis_size(axis)
    initial, last = (max(0, -steps), min(count, count - steps))
    return lax.ppermute(value, axis, [(source, source + steps) for source in range(initial, last)])


def attend_terms(query_grid, bias_grid, key_block, value_block, live, carried):
    kv_local = bias_grid.shape[0]
    key_count = key_block.shape[0]
    logits = (
        jnp.einsum(
            "qgrd,sgd->grqs",
            query_grid,
            key_block.reshape(key_count, kv_local, DH),
            preferred_element_type=jnp.float32,
        )
        * DH ** (-0.5)
        + bias_grid[:, :, None, None]
    )
    keep = jnp.where(live, jax.nn.log_sigmoid(-logits), 0.0)
    after = lax.cumsum(keep, axis=3, reverse=True) - keep + carried[:, :, :, None]
    weight = jnp.where(live, jnp.exp(jax.nn.log_sigmoid(logits) + after), 0.0).astype(jnp.bfloat16)
    partial_mix = jnp.einsum(
        "grqs,sgd->qgrd",
        weight,
        value_block.reshape(key_count, kv_local, DH),
        preferred_element_type=jnp.float32,
    )
    return (partial_mix, jnp.sum(keep, axis=3))


def middle_ring(queries, keys, values, head_bias, documents, w_out, resid, norm_gain):
    tok_count = queries.shape[0]
    kv_local = keys.shape[1] // DH
    group_size = HEADS // KV_HEADS
    sp_count = lax.axis_size("sp")
    sp_index = lax.axis_index("sp")
    query_grid = queries.reshape(tok_count, kv_local, group_size, DH)
    bias_grid = head_bias.reshape(kv_local, group_size)
    doc_here = documents.astype(jnp.bfloat16)
    doc_column = doc_here.reshape(tok_count, 1)
    local_pos = jnp.arange(tok_count, dtype=jnp.int32)
    live_local = (local_pos[None, :] < local_pos[:, None]) & (
        documents[None, :] == documents[:, None]
    )
    zero_carry = jnp.zeros((kv_local, group_size, tok_count), jnp.float32)
    mix_total, carried = attend_terms(query_grid, bias_grid, keys, values, live_local, zero_carry)

    def visit(turn_index, state):
        mix_sum, carry_sum, key_block, value_block, doc_block = state
        key_block, value_block, doc_block = passed_along(
            (key_block, value_block, doc_block), "sp", 1
        )
        live = (doc_block[:, 0][None, :] == doc_here[:, None]) & (sp_index - turn_index >= 0)
        partial_mix, block_keep = attend_terms(
            query_grid, bias_grid, key_block, value_block, live, carry_sum
        )
        return (mix_sum + partial_mix, carry_sum + block_keep, key_block, value_block, doc_block)

    mix_total, carried, key_last, value_last, doc_last = lax.fori_loop(
        1, sp_count, visit, (mix_total, carried, keys, values, doc_column)
    )
    mixed = mix_total.reshape(tok_count, kv_local * group_size * DH).astype(jnp.bfloat16)
    projected = lax.psum_scatter(
        jnp.dot(mixed, w_out, preferred_element_type=jnp.float32).astype(jnp.bfloat16),
        "tp",
        scatter_dimension=0,
        tiled=True,
    ).astype(jnp.float32)
    middle = (resid.astype(jnp.float32) + projected).astype(jnp.bfloat16)
    middle_value = middle.astype(jnp.float32)
    normed = (
        middle_value
        * lax.rsqrt(jnp.mean(middle_value * middle_value, axis=1, keepdims=True) + 1e-06)
        * norm_gain
    ).astype(jnp.bfloat16)
    return middle, normed


def experts_routed(middle, normed, expert_ids, expert_gates, w_gate, w_up, w_down, slot_limit):
    middle_value = middle.astype(jnp.float32)
    sp_count = lax.axis_size("sp")
    tp_count = lax.axis_size("tp")
    row_count = normed.shape[0]
    expert_count = w_gate.shape[0] * sp_count
    flat_ids = expert_ids.reshape(-1)
    onehot_ids = (flat_ids[:, None] == jnp.arange(expert_count, dtype=jnp.int32)[None, :]).astype(
        jnp.int32
    )
    earlier = jnp.cumsum(onehot_ids, axis=0) - onehot_ids
    slot_ids = jnp.sum(earlier * onehot_ids, axis=1)
    target = flat_ids * slot_limit + slot_ids
    placing = (
        jnp.arange(expert_count * slot_limit, dtype=jnp.int32)[:, None] == target[None, :]
    ).astype(jnp.bfloat16)
    by_token = jnp.sum(placing.reshape(expert_count * slot_limit, row_count, TOPK), axis=2)
    outgoing = jnp.dot(by_token, normed, preferred_element_type=jnp.float32).astype(jnp.bfloat16)
    outgoing = outgoing.reshape(expert_count, slot_limit, D)
    arrived = lax.all_to_all(outgoing, "sp", split_axis=0, concat_axis=0, tiled=True)
    gathered = lax.all_gather(arrived, "tp", axis=0, tiled=True)
    expert_rows = gathered.reshape(-1, D)
    gate_value = jnp.dot(expert_rows, w_gate[0], preferred_element_type=jnp.float32)
    up_value = jnp.dot(expert_rows, w_up[0], preferred_element_type=jnp.float32)
    hidden = (jax.nn.silu(gate_value) * up_value).astype(jnp.bfloat16)
    partial_out = jnp.dot(hidden, w_down[0], preferred_element_type=jnp.float32)
    summed = lax.psum_scatter(
        partial_out.reshape(tp_count, sp_count * slot_limit, D).astype(jnp.bfloat16),
        "tp",
        scatter_dimension=0,
        tiled=True,
    ).astype(jnp.float32)
    expert_result = summed.reshape(sp_count, slot_limit, D).astype(jnp.bfloat16)
    returned = lax.all_to_all(expert_result, "sp", split_axis=0, concat_axis=0, tiled=True)
    routed = jnp.dot(placing.T, returned.reshape(-1, D), preferred_element_type=jnp.float32)
    combined = jnp.sum(expert_gates[:, :, None] * routed.reshape(row_count, TOPK, D), axis=1)
    return (middle_value + combined).astype(jnp.bfloat16)


def local(
    queries,
    keys,
    values,
    head_bias,
    documents,
    w_out,
    resid,
    norm_gain,
    expert_ids,
    expert_gates,
    w_gate,
    w_up,
    w_down,
):
    sp_count = lax.axis_size("sp")
    tp_count = lax.axis_size("tp")
    paired = tp_count & (tp_count - 1) == 0
    direct = paired and sp_count * keys.shape[0] <= DIRECT_KEYS and sp_count > 1
    middle_of = middle_direct if direct else middle_ring
    middle, normed = middle_of(
        queries, keys, values, head_bias, documents, w_out, resid, norm_gain
    )
    row_count = normed.shape[0]
    expert_count = w_gate.shape[0] * sp_count
    slot_limit = min(row_count, max(2, 2 * TOPK * row_count // expert_count))
    routing = (middle, normed, expert_ids, expert_gates, w_gate, w_up, w_down)
    if paired and slot_limit == row_count and w_gate.shape[0] == 1 and sp_count > 1:
        return experts_dense(*routing)
    return experts_routed(*routing, slot_limit)


def solution(mesh):
    return jax.shard_map(
        local,
        mesh=mesh,
        in_specs=(
            P(("grp", "sp"), "tp"),
            P(("grp", "sp"), "tp"),
            P(("grp", "sp"), "tp"),
            P("tp"),
            P(("grp", "sp")),
            P("tp", None),
            P(("grp", "sp", "tp"), None),
            P(),
            P(("grp", "sp", "tp"), None),
            P(("grp", "sp", "tp"), None),
            P("sp", None, "tp"),
            P("sp", None, "tp"),
            P("sp", "tp", None),
        ),
        out_specs=P(("grp", "sp", "tp"), None),
        check_vma=False,
    )
```

```python
import functools

import jax
import jax.numpy as jnp
from jax import lax
from jax.experimental import pallas as pl
from jax.experimental.pallas import tpu as pltpu
from jax.sharding import PartitionSpec as P


D = 2048
HEADS = 16
KV_HEADS = 8
DH = 128
TOPK = 2
DOC_ROWS = 16
DIRECT_KEYS = 1024
SMALL = 20 * 2**20
VMEM = pl.BlockSpec(memory_space=pltpu.VMEM)
SMEM = pl.BlockSpec(memory_space=pltpu.SMEM)


def shifted(value, steps, wrap):
    count = lax.axis_size("sp")
    pairs = [(i, (i + steps) % count) for i in range(count) if wrap or 0 <= i + steps < count]
    return lax.ppermute(value, "sp", pairs)


def swapped(value, mask):
    count = lax.axis_size("tp")
    return lax.ppermute(value, "tp", [(i, i ^ mask) for i in range(count)])


def block_terms(q_ref, bias_ref, key_of, value_of, live, carry):
    heads = q_ref.shape[1] // DH
    group = HEADS // KV_HEADS
    rows = q_ref.shape[0]
    parts = []
    for h in range(heads):
        part = lax.dot_general(
            q_ref[:, h * DH : (h + 1) * DH],
            key_of(h // group),
            (((1,), (1,)), ((), ())),
            preferred_element_type=jnp.float32,
        )
        parts.append(part * DH ** (-0.5) + bias_ref[h])
    logits = jnp.concatenate(parts, axis=0)
    live = jnp.concatenate([live] * heads, axis=0)
    soft = jnp.log1p(jnp.exp(-jnp.abs(logits)))
    keep = jnp.where(live, -jnp.maximum(logits, 0.0) - soft, 0.0)
    keys = logits.shape[1]
    later = lax.broadcasted_iota(jnp.int32, (keys, keys), 0) > lax.broadcasted_iota(
        jnp.int32, (keys, keys), 1
    )
    later = later.astype(jnp.float32).astype(jnp.bfloat16)
    high = keep.astype(jnp.bfloat16)
    low = (keep - high.astype(jnp.float32)).astype(jnp.bfloat16)
    after = jnp.dot(high, later, preferred_element_type=jnp.float32) + jnp.dot(
        low, later, preferred_element_type=jnp.float32
    )
    weight = jnp.where(
        live, jnp.exp(jnp.minimum(logits, 0.0) - soft + after + carry), 0.0
    ).astype(jnp.bfloat16)
    mixes = [
        jnp.dot(
            weight[h * rows : (h + 1) * rows], value_of(h // group), preferred_element_type=jnp.float32
        )
        for h in range(heads)
    ]
    return jnp.concatenate(mixes, axis=1), carry + jnp.sum(keep, axis=1, keepdims=True)


def here_kernel(q_ref, k_ref, v_ref, bias_ref, col_ref, row_ref, mix_ref, carry_ref):
    rows = q_ref.shape[0]
    causal = lax.broadcasted_iota(jnp.int32, (rows, rows), 1) < lax.broadcasted_iota(
        jnp.int32, (rows, rows), 0
    )
    live = causal & (col_ref[...] == row_ref[...])
    carry = jnp.zeros((rows * (q_ref.shape[1] // DH), 1), jnp.float32)
    mix, carry = block_terms(
        q_ref,
        bias_ref,
        lambda g: k_ref[:, g * DH : (g + 1) * DH],
        lambda g: v_ref[:, g * DH : (g + 1) * DH],
        live,
        carry,
    )
    mix_ref[...] = mix
    carry_ref[...] = jnp.broadcast_to(carry, carry_ref.shape)


def away_kernel(count, order, place_ref, q_ref, bias_ref, col_ref, mix_ref, carry_ref, w_ref, *refs):
    sent, outs, mixed_ref = refs[:count], refs[count:-1], refs[-1]
    rows = q_ref.shape[0]
    width = q_ref.shape[1] // (HEADS // KV_HEADS)
    mix = mix_ref[...]
    carry = carry_ref[:, 0:1]
    for step, block in enumerate(sent, 1):
        doc_row = block[rows : rows + 1, 0:rows].astype(jnp.float32)
        doc_row = jnp.where(place_ref[0] >= step, doc_row, -1.0)
        live = col_ref[...] == doc_row
        term, carry = block_terms(
            q_ref,
            bias_ref,
            lambda g, block=block: block[0:rows, g * DH : (g + 1) * DH],
            lambda g, block=block: block[0:rows, width + g * DH : width + (g + 1) * DH],
            live,
            carry,
        )
        mix = mix + term
    mixed_ref[...] = mix
    share = rows // len(order)
    for mask, out in zip(order, outs):
        first = pl.multiple_of((place_ref[1] ^ mask) * share, share)
        piece = mixed_ref[pl.ds(first, share), :].astype(jnp.bfloat16)
        out[...] = jnp.dot(piece, w_ref[...], preferred_element_type=jnp.float32).astype(jnp.bfloat16)


def norm_kernel(resid_ref, gain_ref, *refs):
    pieces, middle_ref, normed_ref = refs[:-2], refs[-2], refs[-1]
    total = pieces[0][...].astype(jnp.float32)
    for piece in pieces[1:]:
        total = total + piece[...].astype(jnp.float32)
    middle = (resid_ref[...].astype(jnp.float32) + total).astype(jnp.bfloat16)
    middle_ref[...] = middle
    value = middle.astype(jnp.float32)
    scale = lax.rsqrt(jnp.mean(value * value, axis=1, keepdims=True) + 1e-06)
    normed_ref[...] = (value * scale * gain_ref[...]).astype(jnp.bfloat16)


def expert_kernel(near_ref, far_ref, gate_ref, up_ref, down_ref, kept_ref, sent_ref, held_ref, hidden_ref):
    half = near_ref.shape[0]
    held_ref[:half, :] = near_ref[...]
    held_ref[half:, :] = far_ref[...]
    tile = 256
    for at in range(0, gate_ref.shape[2], tile):
        gate_value = jnp.dot(
            held_ref[...], gate_ref[0, :, at : at + tile], preferred_element_type=jnp.float32
        )
        up_value = jnp.dot(
            held_ref[...], up_ref[0, :, at : at + tile], preferred_element_type=jnp.float32
        )
        hidden = gate_value / (1.0 + jnp.exp(-gate_value)) * up_value
        hidden_ref[:, at : at + tile] = hidden.astype(jnp.bfloat16)
    for at in range(0, down_ref.shape[2], tile):
        result = jnp.dot(
            hidden_ref[...], down_ref[0, :, at : at + tile], preferred_element_type=jnp.float32
        ).astype(jnp.bfloat16)
        kept_ref[:, at : at + tile] = result[:half]
        sent_ref[:, at : at + tile] = result[half:]


def cost(flops, nbytes):
    return pl.CostEstimate(flops=flops, bytes_accessed=nbytes, transcendentals=0)


def middle_direct(queries, keys, values, head_bias, documents, w_out, resid, norm_gain):
    rows, width = queries.shape
    kv_width = keys.shape[1]
    sp_count = lax.axis_size("sp")
    tp_count = lax.axis_size("tp")
    doc_real = documents.astype(jnp.bfloat16)
    doc_rows = jnp.zeros((DOC_ROWS, 2 * kv_width), jnp.bfloat16)
    doc_rows = doc_rows.at[0, :rows].set(doc_real)
    packed = jnp.concatenate([jnp.concatenate([keys, values], axis=1), doc_rows], axis=0)
    sent = [shifted(packed, steps, False) for steps in range(1, sp_count)]
    col = documents.astype(jnp.float32).reshape(rows, 1)
    row = documents.astype(jnp.float32).reshape(1, rows)
    heads = width // DH
    mix, carry = pl.pallas_call(
        here_kernel,
        out_shape=(
            jax.ShapeDtypeStruct((rows, width), jnp.float32),
            jax.ShapeDtypeStruct((rows * heads, DH), jnp.float32),
        ),
        in_specs=[VMEM, VMEM, VMEM, SMEM, VMEM, VMEM],
        out_specs=(VMEM, VMEM),
        cost_estimate=cost(6 * 10**9, 10**6),
        compiler_params=pltpu.CompilerParams(vmem_limit_bytes=SMALL),
        name="attend_here",
    )(queries, keys, values, head_bias, col, row)
    place = jnp.stack([lax.axis_index("sp"), lax.axis_index("tp")]).astype(jnp.int32)
    order = list(range(tp_count))
    share = rows // tp_count
    pieces = pl.pallas_call(
        functools.partial(away_kernel, sp_count - 1, order),
        out_shape=[jax.ShapeDtypeStruct((share, D), jnp.bfloat16)] * tp_count,
        in_specs=[SMEM, VMEM, SMEM, VMEM, VMEM, VMEM, VMEM] + [VMEM] * (sp_count - 1),
        out_specs=[VMEM] * tp_count,
        scratch_shapes=[pltpu.VMEM((rows, width), jnp.float32)],
        cost_estimate=cost(10 * 10**9, 4 * 10**6),
        compiler_params=pltpu.CompilerParams(vmem_limit_bytes=SMALL),
        name="attend_away",
    )(place, queries, head_bias, col, mix, carry, w_out, *sent)
    arrived = [pieces[0]] + [swapped(pieces[mask], mask) for mask in order[:0:-1]]
    return pl.pallas_call(
        norm_kernel,
        out_shape=[jax.ShapeDtypeStruct((share, D), jnp.bfloat16)] * 2,
        in_specs=[VMEM] * (2 + tp_count),
        out_specs=[VMEM] * 2,
        cost_estimate=cost(10**8, 10**6),
        compiler_params=pltpu.CompilerParams(vmem_limit_bytes=SMALL),
        name="middle_norm",
    )(resid, norm_gain.reshape(1, D), *arrived)


def experts_dense(middle, normed, expert_ids, expert_gates, w_gate, w_up, w_down):
    rows = normed.shape[0]
    sp_count = lax.axis_size("sp")
    tp_count = lax.axis_size("tp")
    masks = [1 << bit for bit in range(tp_count.bit_length() - 1)]
    steps = [0] + [s for pair in zip(range(1, sp_count), range(sp_count - 1, 0, -1)) for s in pair]
    steps = list(dict.fromkeys(steps))
    half = (len(steps) + 1) // 2
    moved = {0: normed}
    for s in steps[1:]:
        moved[s] = shifted(normed, s, True)
    pieces = {}
    for chunk in (steps[:half], steps[half:]):
        held = jnp.concatenate([moved[s] for s in chunk], axis=0)
        for mask in masks[:0:-1]:
            other = swapped(held, mask)
            held = jnp.concatenate([held, other], axis=0)
        far = swapped(held, 1)
        count = held.shape[0]
        result, leaving = pl.pallas_call(
            expert_kernel,
            out_shape=[jax.ShapeDtypeStruct((count, D), jnp.bfloat16)] * 2,
            in_specs=[VMEM] * 5,
            out_specs=[VMEM] * 2,
            scratch_shapes=[
                pltpu.VMEM((2 * count, D), jnp.bfloat16),
                pltpu.VMEM((2 * count, w_gate.shape[2]), jnp.bfloat16),
            ],
            compiler_params=pltpu.CompilerParams(vmem_limit_bytes=32 * 2**20),
            cost_estimate=cost(12 * count * D * w_gate.shape[2], 12 * 10**6),
        )(held, far, w_gate, w_up, w_down)
        for mask in masks:
            if mask > 1:
                kept = result.shape[0] // 2
                result, leaving = result[:kept], result[kept:]
            other = swapped(leaving, mask)
            result = (result.astype(jnp.float32) + other.astype(jnp.float32)).astype(jnp.bfloat16)
        for at, s in enumerate(chunk):
            pieces[s] = result[at * rows : (at + 1) * rows]
    own = lax.axis_index("sp")
    total = middle.astype(jnp.float32)
    combined = jnp.zeros_like(total)
    for s in steps:
        piece = pieces[s] if s == 0 else shifted(pieces[s], -s, True)
        chosen = expert_ids == (own + s) % sp_count
        scale = jnp.sum(jnp.where(chosen, expert_gates, 0.0), axis=1, keepdims=True)
        combined = combined + scale * piece.astype(jnp.float32)
    return (total + combined).astype(jnp.bfloat16)


def passed_along(value, axis, steps):
    count = lax.axis_size(axis)
    initial, last = (max(0, -steps), min(count, count - steps))
    return lax.ppermute(value, axis, [(source, source + steps) for source in range(initial, last)])


def attend_terms(query_grid, bias_grid, key_block, value_block, live, carried):
    kv_local = bias_grid.shape[0]
    key_count = key_block.shape[0]
    logits = (
        jnp.einsum(
            "qgrd,sgd->grqs",
            query_grid,
            key_block.reshape(key_count, kv_local, DH),
            preferred_element_type=jnp.float32,
        )
        * DH ** (-0.5)
        + bias_grid[:, :, None, None]
    )
    keep = jnp.where(live, jax.nn.log_sigmoid(-logits), 0.0)
    after = lax.cumsum(keep, axis=3, reverse=True) - keep + carried[:, :, :, None]
    weight = jnp.where(live, jnp.exp(jax.nn.log_sigmoid(logits) + after), 0.0).astype(jnp.bfloat16)
    partial_mix = jnp.einsum(
        "grqs,sgd->qgrd",
        weight,
        value_block.reshape(key_count, kv_local, DH),
        preferred_element_type=jnp.float32,
    )
    return (partial_mix, jnp.sum(keep, axis=3))


def middle_ring(queries, keys, values, head_bias, documents, w_out, resid, norm_gain):
    tok_count = queries.shape[0]
    kv_local = keys.shape[1] // DH
    group_size = HEADS // KV_HEADS
    sp_count = lax.axis_size("sp")
    sp_index = lax.axis_index("sp")
    query_grid = queries.reshape(tok_count, kv_local, group_size, DH)
    bias_grid = head_bias.reshape(kv_local, group_size)
    doc_here = documents.astype(jnp.bfloat16)
    doc_column = doc_here.reshape(tok_count, 1)
    local_pos = jnp.arange(tok_count, dtype=jnp.int32)
    live_local = (local_pos[None, :] < local_pos[:, None]) & (
        documents[None, :] == documents[:, None]
    )
    zero_carry = jnp.zeros((kv_local, group_size, tok_count), jnp.float32)
    mix_total, carried = attend_terms(query_grid, bias_grid, keys, values, live_local, zero_carry)

    def visit(turn_index, state):
        mix_sum, carry_sum, key_block, value_block, doc_block = state
        key_block, value_block, doc_block = passed_along(
            (key_block, value_block, doc_block), "sp", 1
        )
        live = (doc_block[:, 0][None, :] == doc_here[:, None]) & (sp_index - turn_index >= 0)
        partial_mix, block_keep = attend_terms(
            query_grid, bias_grid, key_block, value_block, live, carry_sum
        )
        return (mix_sum + partial_mix, carry_sum + block_keep, key_block, value_block, doc_block)

    mix_total, carried, _, _, _ = lax.fori_loop(
        1, sp_count, visit, (mix_total, carried, keys, values, doc_column)
    )
    mixed = mix_total.reshape(tok_count, kv_local * group_size * DH).astype(jnp.bfloat16)
    projected = lax.psum_scatter(
        jnp.dot(mixed, w_out, preferred_element_type=jnp.float32).astype(jnp.bfloat16),
        "tp",
        scatter_dimension=0,
        tiled=True,
    ).astype(jnp.float32)
    middle = (resid.astype(jnp.float32) + projected).astype(jnp.bfloat16)
    middle_value = middle.astype(jnp.float32)
    normed = (
        middle_value
        * lax.rsqrt(jnp.mean(middle_value * middle_value, axis=1, keepdims=True) + 1e-06)
        * norm_gain
    ).astype(jnp.bfloat16)
    return middle, normed


def experts_routed(middle, normed, expert_ids, expert_gates, w_gate, w_up, w_down, slot_limit):
    middle_value = middle.astype(jnp.float32)
    sp_count = lax.axis_size("sp")
    tp_count = lax.axis_size("tp")
    row_count = normed.shape[0]
    expert_count = w_gate.shape[0] * sp_count
    flat_ids = expert_ids.reshape(-1)
    onehot_ids = (flat_ids[:, None] == jnp.arange(expert_count, dtype=jnp.int32)[None, :]).astype(
        jnp.int32
    )
    earlier = jnp.cumsum(onehot_ids, axis=0) - onehot_ids
    slot_ids = jnp.sum(earlier * onehot_ids, axis=1)
    target = flat_ids * slot_limit + slot_ids
    placing = (
        jnp.arange(expert_count * slot_limit, dtype=jnp.int32)[:, None] == target[None, :]
    ).astype(jnp.bfloat16)
    by_token = jnp.sum(placing.reshape(expert_count * slot_limit, row_count, TOPK), axis=2)
    outgoing = jnp.dot(by_token, normed, preferred_element_type=jnp.float32).astype(jnp.bfloat16)
    outgoing = outgoing.reshape(expert_count, slot_limit, D)
    arrived = lax.all_to_all(outgoing, "sp", split_axis=0, concat_axis=0, tiled=True)
    gathered = lax.all_gather(arrived, "tp", axis=0, tiled=True)
    expert_rows = gathered.reshape(-1, D)
    gate_value = jnp.dot(expert_rows, w_gate[0], preferred_element_type=jnp.float32)
    up_value = jnp.dot(expert_rows, w_up[0], preferred_element_type=jnp.float32)
    hidden = (jax.nn.silu(gate_value) * up_value).astype(jnp.bfloat16)
    partial_out = jnp.dot(hidden, w_down[0], preferred_element_type=jnp.float32)
    summed = lax.psum_scatter(
        partial_out.reshape(tp_count, sp_count * slot_limit, D).astype(jnp.bfloat16),
        "tp",
        scatter_dimension=0,
        tiled=True,
    ).astype(jnp.float32)
    expert_result = summed.reshape(sp_count, slot_limit, D).astype(jnp.bfloat16)
    returned = lax.all_to_all(expert_result, "sp", split_axis=0, concat_axis=0, tiled=True)
    routed = jnp.dot(placing.T, returned.reshape(-1, D), preferred_element_type=jnp.float32)
    combined = jnp.sum(expert_gates[:, :, None] * routed.reshape(row_count, TOPK, D), axis=1)
    return (middle_value + combined).astype(jnp.bfloat16)


def local(
    queries,
    keys,
    values,
    head_bias,
    documents,
    w_out,
    resid,
    norm_gain,
    expert_ids,
    expert_gates,
    w_gate,
    w_up,
    w_down,
):
    sp_count = lax.axis_size("sp")
    tp_count = lax.axis_size("tp")
    paired = tp_count & (tp_count - 1) == 0
    direct = paired and sp_count * keys.shape[0] <= DIRECT_KEYS and sp_count > 1
    middle_of = middle_direct if direct else middle_ring
    middle, normed = middle_of(
        queries, keys, values, head_bias, documents, w_out, resid, norm_gain
    )
    row_count = normed.shape[0]
    expert_count = w_gate.shape[0] * sp_count
    slot_limit = min(row_count, max(2, 2 * TOPK * row_count // expert_count))
    routing = (middle, normed, expert_ids, expert_gates, w_gate, w_up, w_down)
    if paired and slot_limit == row_count and w_gate.shape[0] == 1 and sp_count > 1:
        return experts_dense(*routing)
    return experts_routed(*routing, slot_limit)


def solution(mesh):
    return jax.shard_map(
        local,
        mesh=mesh,
        in_specs=(
            P(("grp", "sp"), "tp"),
            P(("grp", "sp"), "tp"),
            P(("grp", "sp"), "tp"),
            P("tp"),
            P(("grp", "sp")),
            P("tp", None),
            P(("grp", "sp", "tp"), None),
            P(),
            P(("grp", "sp", "tp"), None),
            P(("grp", "sp", "tp"), None),
            P("sp", None, "tp"),
            P("sp", None, "tp"),
            P("sp", "tp", None),
        ),
        out_specs=P(("grp", "sp", "tp"), None),
        check_vma=False,
    )
```

```python
import functools

import jax
import jax.numpy as jnp
from jax import lax
from jax.experimental import pallas as pl
from jax.experimental.pallas import tpu as pltpu
from jax.sharding import PartitionSpec as P


D = 2048
HEADS = 16
KV_HEADS = 8
DH = 128
TOPK = 2
DOC_ROWS = 8
DIRECT_KEYS = 1024
SMALL = 20 * 2**20
VMEM = pl.BlockSpec(memory_space=pltpu.VMEM)
SMEM = pl.BlockSpec(memory_space=pltpu.SMEM)


def shifted(value, steps, wrap):
    count = lax.axis_size("sp")
    pairs = [(i, (i + steps) % count) for i in range(count) if wrap or 0 <= i + steps < count]
    return lax.ppermute(value, "sp", pairs)


def swapped(value, mask):
    count = lax.axis_size("tp")
    return lax.ppermute(value, "tp", [(i, i ^ mask) for i in range(count)])


def block_terms(q_ref, bias_ref, key_of, value_of, live, carry):
    heads = q_ref.shape[1] // DH
    group = HEADS // KV_HEADS
    rows = q_ref.shape[0]
    parts = []
    for h in range(heads):
        part = lax.dot_general(
            q_ref[:, h * DH : (h + 1) * DH],
            key_of(h // group),
            (((1,), (1,)), ((), ())),
            preferred_element_type=jnp.float32,
        )
        parts.append(part * DH ** (-0.5) + bias_ref[h])
    logits = jnp.concatenate(parts, axis=0)
    live = jnp.concatenate([live] * heads, axis=0)
    soft = jnp.log1p(jnp.exp(-jnp.abs(logits)))
    keep = jnp.where(live, -jnp.maximum(logits, 0.0) - soft, 0.0)
    keys = logits.shape[1]
    later = lax.broadcasted_iota(jnp.int32, (keys, keys), 0) > lax.broadcasted_iota(
        jnp.int32, (keys, keys), 1
    )
    later = later.astype(jnp.float32).astype(jnp.bfloat16)
    high = keep.astype(jnp.bfloat16)
    low = (keep - high.astype(jnp.float32)).astype(jnp.bfloat16)
    after = jnp.dot(high, later, preferred_element_type=jnp.float32) + jnp.dot(
        low, later, preferred_element_type=jnp.float32
    )
    weight = jnp.where(
        live, jnp.exp(jnp.minimum(logits, 0.0) - soft + after + carry), 0.0
    ).astype(jnp.bfloat16)
    mixes = [
        jnp.dot(
            weight[h * rows : (h + 1) * rows], value_of(h // group), preferred_element_type=jnp.float32
        )
        for h in range(heads)
    ]
    return jnp.concatenate(mixes, axis=1), carry + jnp.sum(keep, axis=1, keepdims=True)


def here_kernel(q_ref, k_ref, v_ref, bias_ref, col_ref, row_ref, mix_ref, carry_ref):
    rows = q_ref.shape[0]
    causal = lax.broadcasted_iota(jnp.int32, (rows, rows), 1) < lax.broadcasted_iota(
        jnp.int32, (rows, rows), 0
    )
    live = causal & (col_ref[...] == row_ref[...])
    carry = jnp.zeros((rows * (q_ref.shape[1] // DH), 1), jnp.float32)
    mix, carry = block_terms(
        q_ref,
        bias_ref,
        lambda g: k_ref[:, g * DH : (g + 1) * DH],
        lambda g: v_ref[:, g * DH : (g + 1) * DH],
        live,
        carry,
    )
    mix_ref[...] = mix
    carry_ref[...] = jnp.broadcast_to(carry, carry_ref.shape)


def away_kernel(count, order, place_ref, q_ref, bias_ref, col_ref, mix_ref, carry_ref, w_ref, *refs):
    sent, outs, mixed_ref = refs[:count], refs[count:-1], refs[-1]
    rows = q_ref.shape[0]
    width = q_ref.shape[1] // (HEADS // KV_HEADS)
    mix = mix_ref[...]
    carry = carry_ref[:, 0:1]
    for step, block in enumerate(sent, 1):
        doc_row = block[rows : rows + 1, 0:rows].astype(jnp.float32)
        doc_row = jnp.where(place_ref[0] >= step, doc_row, -1.0)
        live = col_ref[...] == doc_row
        term, carry = block_terms(
            q_ref,
            bias_ref,
            lambda g, block=block: block[0:rows, g * DH : (g + 1) * DH],
            lambda g, block=block: block[0:rows, width + g * DH : width + (g + 1) * DH],
            live,
            carry,
        )
        mix = mix + term
    mixed_ref[...] = mix
    share = rows // len(order)
    for mask, out in zip(order, outs):
        first = pl.multiple_of((place_ref[1] ^ mask) * share, share)
        piece = mixed_ref[pl.ds(first, share), :].astype(jnp.bfloat16)
        out[...] = jnp.dot(piece, w_ref[...], preferred_element_type=jnp.float32).astype(jnp.bfloat16)


def norm_kernel(resid_ref, gain_ref, *refs):
    pieces, middle_ref, normed_ref = refs[:-2], refs[-2], refs[-1]
    total = pieces[0][...].astype(jnp.float32)
    for piece in pieces[1:]:
        total = total + piece[...].astype(jnp.float32)
    middle = (resid_ref[...].astype(jnp.float32) + total).astype(jnp.bfloat16)
    middle_ref[...] = middle
    value = middle.astype(jnp.float32)
    scale = lax.rsqrt(jnp.mean(value * value, axis=1, keepdims=True) + 1e-06)
    normed_ref[...] = (value * scale * gain_ref[...]).astype(jnp.bfloat16)


def expert_kernel(near_ref, far_ref, gate_ref, up_ref, down_ref, kept_ref, sent_ref, held_ref, hidden_ref):
    half = near_ref.shape[0]
    held_ref[:half, :] = near_ref[...]
    held_ref[half:, :] = far_ref[...]
    tile = 256
    for at in range(0, gate_ref.shape[2], tile):
        gate_value = jnp.dot(
            held_ref[...], gate_ref[0, :, at : at + tile], preferred_element_type=jnp.float32
        )
        up_value = jnp.dot(
            held_ref[...], up_ref[0, :, at : at + tile], preferred_element_type=jnp.float32
        )
        hidden = gate_value / (1.0 + jnp.exp(-gate_value)) * up_value
        hidden_ref[:, at : at + tile] = hidden.astype(jnp.bfloat16)
    for at in range(0, down_ref.shape[2], tile):
        result = jnp.dot(
            hidden_ref[...], down_ref[0, :, at : at + tile], preferred_element_type=jnp.float32
        ).astype(jnp.bfloat16)
        kept_ref[:, at : at + tile] = result[:half]
        sent_ref[:, at : at + tile] = result[half:]


def cost(flops, nbytes):
    return pl.CostEstimate(flops=flops, bytes_accessed=nbytes, transcendentals=0)


def middle_direct(queries, keys, values, head_bias, documents, w_out, resid, norm_gain):
    rows, width = queries.shape
    kv_width = keys.shape[1]
    sp_count = lax.axis_size("sp")
    tp_count = lax.axis_size("tp")
    doc_real = documents.astype(jnp.bfloat16)
    doc_rows = jnp.zeros((DOC_ROWS, 2 * kv_width), jnp.bfloat16)
    doc_rows = doc_rows.at[0, :rows].set(doc_real)
    packed = jnp.concatenate([jnp.concatenate([keys, values], axis=1), doc_rows], axis=0)
    sent = [shifted(packed, steps, False) for steps in range(1, sp_count)]
    col = documents.astype(jnp.float32).reshape(rows, 1)
    row = documents.astype(jnp.float32).reshape(1, rows)
    heads = width // DH
    mix, carry = pl.pallas_call(
        here_kernel,
        out_shape=(
            jax.ShapeDtypeStruct((rows, width), jnp.float32),
            jax.ShapeDtypeStruct((rows * heads, DH), jnp.float32),
        ),
        in_specs=[VMEM, VMEM, VMEM, SMEM, VMEM, VMEM],
        out_specs=(VMEM, VMEM),
        cost_estimate=cost(6 * 10**9, 10**6),
        name="attend_here",
    )(queries, keys, values, head_bias, col, row)
    place = jnp.stack([lax.axis_index("sp"), lax.axis_index("tp")]).astype(jnp.int32)
    order = list(range(tp_count))
    share = rows // tp_count
    pieces = pl.pallas_call(
        functools.partial(away_kernel, sp_count - 1, order),
        out_shape=[jax.ShapeDtypeStruct((share, D), jnp.bfloat16)] * tp_count,
        in_specs=[SMEM, VMEM, SMEM, VMEM, VMEM, VMEM, VMEM] + [VMEM] * (sp_count - 1),
        out_specs=[VMEM] * tp_count,
        scratch_shapes=[pltpu.VMEM((rows, width), jnp.float32)],
        cost_estimate=cost(10 * 10**9, 4 * 10**6),
        compiler_params=pltpu.CompilerParams(vmem_limit_bytes=SMALL),
        name="attend_away",
    )(place, queries, head_bias, col, mix, carry, w_out, *sent)
    arrived = [pieces[0]] + [swapped(pieces[mask], mask) for mask in order[:0:-1]]
    return pl.pallas_call(
        norm_kernel,
        out_shape=[jax.ShapeDtypeStruct((share, D), jnp.bfloat16)] * 2,
        in_specs=[VMEM] * (2 + tp_count),
        out_specs=[VMEM] * 2,
        cost_estimate=cost(10**8, 10**6),
        compiler_params=pltpu.CompilerParams(vmem_limit_bytes=SMALL),
        name="middle_norm",
    )(resid, norm_gain.reshape(1, D), *arrived)


def experts_dense(middle, normed, expert_ids, expert_gates, w_gate, w_up, w_down):
    rows = normed.shape[0]
    sp_count = lax.axis_size("sp")
    tp_count = lax.axis_size("tp")
    masks = [1 << bit for bit in range(tp_count.bit_length() - 1)]
    steps = [0] + [s for pair in zip(range(1, sp_count), range(sp_count - 1, 0, -1)) for s in pair]
    steps = list(dict.fromkeys(steps))
    chunks = [steps[:1]] + [steps[at : at + 2] for at in range(1, len(steps), 2)]
    moved = {0: normed}
    for chunk in chunks[1:]:
        for s in chunk:
            moved[s] = shifted(normed, s, True)
    pieces = {}
    for at, chunk in enumerate(chunks):
        held = jnp.concatenate([moved[s] for s in chunk], axis=0)
        for mask in masks[:0:-1]:
            other = swapped(held, mask)
            held = jnp.concatenate([held, other], axis=0)
        far = swapped(held, 1)
        count = held.shape[0]
        result, leaving = pl.pallas_call(
            expert_kernel,
            out_shape=[jax.ShapeDtypeStruct((count, D), jnp.bfloat16)] * 2,
            in_specs=[VMEM] * 5,
            out_specs=[VMEM] * 2,
            scratch_shapes=[
                pltpu.VMEM((2 * count, D), jnp.bfloat16),
                pltpu.VMEM((2 * count, w_gate.shape[2]), jnp.bfloat16),
            ],
            compiler_params=pltpu.CompilerParams(vmem_limit_bytes=32 * 2**20),
            cost_estimate=cost(12 * count * D * w_gate.shape[2], 12 * 10**6),
        )(held, far, w_gate, w_up, w_down)
        for mask in masks:
            if mask > 1:
                kept = result.shape[0] // 2
                result, leaving = result[:kept], result[kept:]
            other = swapped(leaving, mask)
            result = (result.astype(jnp.float32) + other.astype(jnp.float32)).astype(jnp.bfloat16)
        for at, s in enumerate(chunk):
            pieces[s] = result[at * rows : (at + 1) * rows]
    own = lax.axis_index("sp")
    total = middle.astype(jnp.float32)
    combined = jnp.zeros_like(total)
    for s in steps:
        piece = pieces[s] if s == 0 else shifted(pieces[s], -s, True)
        chosen = expert_ids == (own + s) % sp_count
        scale = jnp.sum(jnp.where(chosen, expert_gates, 0.0), axis=1, keepdims=True)
        combined = combined + scale * piece.astype(jnp.float32)
    return (total + combined).astype(jnp.bfloat16)


def passed_along(value, axis, steps):
    count = lax.axis_size(axis)
    initial, last = (max(0, -steps), min(count, count - steps))
    return lax.ppermute(value, axis, [(source, source + steps) for source in range(initial, last)])


def attend_terms(query_grid, bias_grid, key_block, value_block, live, carried):
    kv_local = bias_grid.shape[0]
    key_count = key_block.shape[0]
    logits = (
        jnp.einsum(
            "qgrd,sgd->grqs",
            query_grid,
            key_block.reshape(key_count, kv_local, DH),
            preferred_element_type=jnp.float32,
        )
        * DH ** (-0.5)
        + bias_grid[:, :, None, None]
    )
    keep = jnp.where(live, jax.nn.log_sigmoid(-logits), 0.0)
    after = lax.cumsum(keep, axis=3, reverse=True) - keep + carried[:, :, :, None]
    weight = jnp.where(live, jnp.exp(jax.nn.log_sigmoid(logits) + after), 0.0).astype(jnp.bfloat16)
    partial_mix = jnp.einsum(
        "grqs,sgd->qgrd",
        weight,
        value_block.reshape(key_count, kv_local, DH),
        preferred_element_type=jnp.float32,
    )
    return (partial_mix, jnp.sum(keep, axis=3))


def middle_ring(queries, keys, values, head_bias, documents, w_out, resid, norm_gain):
    tok_count = queries.shape[0]
    kv_local = keys.shape[1] // DH
    group_size = HEADS // KV_HEADS
    sp_count = lax.axis_size("sp")
    sp_index = lax.axis_index("sp")
    query_grid = queries.reshape(tok_count, kv_local, group_size, DH)
    bias_grid = head_bias.reshape(kv_local, group_size)
    doc_here = documents.astype(jnp.bfloat16)
    doc_column = doc_here.reshape(tok_count, 1)
    local_pos = jnp.arange(tok_count, dtype=jnp.int32)
    live_local = (local_pos[None, :] < local_pos[:, None]) & (
        documents[None, :] == documents[:, None]
    )
    zero_carry = jnp.zeros((kv_local, group_size, tok_count), jnp.float32)
    mix_total, carried = attend_terms(query_grid, bias_grid, keys, values, live_local, zero_carry)

    def visit(turn_index, state):
        mix_sum, carry_sum, key_block, value_block, doc_block = state
        key_block, value_block, doc_block = passed_along(
            (key_block, value_block, doc_block), "sp", 1
        )
        live = (doc_block[:, 0][None, :] == doc_here[:, None]) & (sp_index - turn_index >= 0)
        partial_mix, block_keep = attend_terms(
            query_grid, bias_grid, key_block, value_block, live, carry_sum
        )
        return (mix_sum + partial_mix, carry_sum + block_keep, key_block, value_block, doc_block)

    mix_total, carried, _, _, _ = lax.fori_loop(
        1, sp_count, visit, (mix_total, carried, keys, values, doc_column)
    )
    mixed = mix_total.reshape(tok_count, kv_local * group_size * DH).astype(jnp.bfloat16)
    projected = lax.psum_scatter(
        jnp.dot(mixed, w_out, preferred_element_type=jnp.float32).astype(jnp.bfloat16),
        "tp",
        scatter_dimension=0,
        tiled=True,
    ).astype(jnp.float32)
    middle = (resid.astype(jnp.float32) + projected).astype(jnp.bfloat16)
    middle_value = middle.astype(jnp.float32)
    normed = (
        middle_value
        * lax.rsqrt(jnp.mean(middle_value * middle_value, axis=1, keepdims=True) + 1e-06)
        * norm_gain
    ).astype(jnp.bfloat16)
    return middle, normed


def experts_routed(middle, normed, expert_ids, expert_gates, w_gate, w_up, w_down, slot_limit):
    middle_value = middle.astype(jnp.float32)
    sp_count = lax.axis_size("sp")
    tp_count = lax.axis_size("tp")
    row_count = normed.shape[0]
    expert_count = w_gate.shape[0] * sp_count
    flat_ids = expert_ids.reshape(-1)
    onehot_ids = (flat_ids[:, None] == jnp.arange(expert_count, dtype=jnp.int32)[None, :]).astype(
        jnp.int32
    )
    earlier = jnp.cumsum(onehot_ids, axis=0) - onehot_ids
    slot_ids = jnp.sum(earlier * onehot_ids, axis=1)
    target = flat_ids * slot_limit + slot_ids
    placing = (
        jnp.arange(expert_count * slot_limit, dtype=jnp.int32)[:, None] == target[None, :]
    ).astype(jnp.bfloat16)
    by_token = jnp.sum(placing.reshape(expert_count * slot_limit, row_count, TOPK), axis=2)
    outgoing = jnp.dot(by_token, normed, preferred_element_type=jnp.float32).astype(jnp.bfloat16)
    outgoing = outgoing.reshape(expert_count, slot_limit, D)
    arrived = lax.all_to_all(outgoing, "sp", split_axis=0, concat_axis=0, tiled=True)
    gathered = lax.all_gather(arrived, "tp", axis=0, tiled=True)
    expert_rows = gathered.reshape(-1, D)
    gate_value = jnp.dot(expert_rows, w_gate[0], preferred_element_type=jnp.float32)
    up_value = jnp.dot(expert_rows, w_up[0], preferred_element_type=jnp.float32)
    hidden = (jax.nn.silu(gate_value) * up_value).astype(jnp.bfloat16)
    partial_out = jnp.dot(hidden, w_down[0], preferred_element_type=jnp.float32)
    summed = lax.psum_scatter(
        partial_out.reshape(tp_count, sp_count * slot_limit, D).astype(jnp.bfloat16),
        "tp",
        scatter_dimension=0,
        tiled=True,
    ).astype(jnp.float32)
    expert_result = summed.reshape(sp_count, slot_limit, D).astype(jnp.bfloat16)
    returned = lax.all_to_all(expert_result, "sp", split_axis=0, concat_axis=0, tiled=True)
    routed = jnp.dot(placing.T, returned.reshape(-1, D), preferred_element_type=jnp.float32)
    combined = jnp.sum(expert_gates[:, :, None] * routed.reshape(row_count, TOPK, D), axis=1)
    return (middle_value + combined).astype(jnp.bfloat16)


def local(
    queries,
    keys,
    values,
    head_bias,
    documents,
    w_out,
    resid,
    norm_gain,
    expert_ids,
    expert_gates,
    w_gate,
    w_up,
    w_down,
):
    sp_count = lax.axis_size("sp")
    tp_count = lax.axis_size("tp")
    paired = tp_count & (tp_count - 1) == 0
    direct = paired and sp_count * keys.shape[0] <= DIRECT_KEYS and sp_count > 1
    middle_of = middle_direct if direct else middle_ring
    middle, normed = middle_of(
        queries, keys, values, head_bias, documents, w_out, resid, norm_gain
    )
    row_count = normed.shape[0]
    expert_count = w_gate.shape[0] * sp_count
    slot_limit = min(row_count, max(2, 2 * TOPK * row_count // expert_count))
    routing = (middle, normed, expert_ids, expert_gates, w_gate, w_up, w_down)
    if paired and slot_limit == row_count and w_gate.shape[0] == 1 and sp_count > 1:
        return experts_dense(*routing)
    return experts_routed(*routing, slot_limit)


def solution(mesh):
    return jax.shard_map(
        local,
        mesh=mesh,
        in_specs=(
            P(("grp", "sp"), "tp"),
            P(("grp", "sp"), "tp"),
            P(("grp", "sp"), "tp"),
            P("tp"),
            P(("grp", "sp")),
            P("tp", None),
            P(("grp", "sp", "tp"), None),
            P(),
            P(("grp", "sp", "tp"), None),
            P(("grp", "sp", "tp"), None),
            P("sp", None, "tp"),
            P("sp", None, "tp"),
            P("sp", "tp", None),
        ),
        out_specs=P(("grp", "sp", "tp"), None),
        check_vma=False,
    )
```

```python
import functools

import jax
import jax.numpy as jnp
from jax import lax
from jax.experimental import pallas as pl
from jax.experimental.pallas import tpu as pltpu
from jax.sharding import PartitionSpec as P


D = 2048
HEADS = 16
KV_HEADS = 8
DH = 128
TOPK = 2
DOC_ROWS = 8
DIRECT_KEYS = 1024
SMALL = 20 * 2**20
VMEM = pl.BlockSpec(memory_space=pltpu.VMEM)
SMEM = pl.BlockSpec(memory_space=pltpu.SMEM)


def shifted(value, steps, wrap):
    count = lax.axis_size("sp")
    pairs = [(i, (i + steps) % count) for i in range(count) if wrap or 0 <= i + steps < count]
    return lax.ppermute(value, "sp", pairs)


def swapped(value, mask):
    count = lax.axis_size("tp")
    return lax.ppermute(value, "tp", [(i, i ^ mask) for i in range(count)])


def block_terms(q_ref, bias_ref, key_of, value_of, live, carry):
    heads = q_ref.shape[1] // DH
    group = HEADS // KV_HEADS
    rows = q_ref.shape[0]
    parts = []
    for h in range(heads):
        part = lax.dot_general(
            q_ref[:, h * DH : (h + 1) * DH],
            key_of(h // group),
            (((1,), (1,)), ((), ())),
            preferred_element_type=jnp.float32,
        )
        parts.append(part * DH ** (-0.5) + bias_ref[h])
    logits = jnp.concatenate(parts, axis=0)
    live = jnp.concatenate([live] * heads, axis=0)
    soft = jnp.log1p(jnp.exp(-jnp.abs(logits)))
    keep = jnp.where(live, -jnp.maximum(logits, 0.0) - soft, 0.0)
    keys = logits.shape[1]
    later = lax.broadcasted_iota(jnp.int32, (keys, keys), 0) > lax.broadcasted_iota(
        jnp.int32, (keys, keys), 1
    )
    later = later.astype(jnp.float32).astype(jnp.bfloat16)
    high = keep.astype(jnp.bfloat16)
    low = (keep - high.astype(jnp.float32)).astype(jnp.bfloat16)
    after = jnp.dot(high, later, preferred_element_type=jnp.float32) + jnp.dot(
        low, later, preferred_element_type=jnp.float32
    )
    weight = jnp.where(
        live, jnp.exp(jnp.minimum(logits, 0.0) - soft + after + carry), 0.0
    ).astype(jnp.bfloat16)
    mixes = [
        jnp.dot(
            weight[h * rows : (h + 1) * rows], value_of(h // group), preferred_element_type=jnp.float32
        )
        for h in range(heads)
    ]
    return jnp.concatenate(mixes, axis=1), carry + jnp.sum(keep, axis=1, keepdims=True)


def here_kernel(q_ref, k_ref, v_ref, bias_ref, col_ref, row_ref, mix_ref, carry_ref):
    rows = q_ref.shape[0]
    causal = lax.broadcasted_iota(jnp.int32, (rows, rows), 1) < lax.broadcasted_iota(
        jnp.int32, (rows, rows), 0
    )
    live = causal & (col_ref[...] == row_ref[...])
    carry = jnp.zeros((rows * (q_ref.shape[1] // DH), 1), jnp.float32)
    mix, carry = block_terms(
        q_ref,
        bias_ref,
        lambda g: k_ref[:, g * DH : (g + 1) * DH],
        lambda g: v_ref[:, g * DH : (g + 1) * DH],
        live,
        carry,
    )
    mix_ref[...] = mix
    lanes = [carry[at : at + rows] for at in range(0, carry.shape[0], rows)]
    lanes.append(jnp.zeros((rows, DH - len(lanes)), jnp.float32))
    carry_ref[...] = jnp.concatenate(lanes, axis=1)


def away_kernel(count, order, place_ref, q_ref, bias_ref, col_ref, mix_ref, carry_ref, w_ref, *refs):
    sent, outs, mixed_ref = refs[:count], refs[count:-1], refs[-1]
    rows = q_ref.shape[0]
    width = q_ref.shape[1] // (HEADS // KV_HEADS)
    mix = mix_ref[...]
    heads = q_ref.shape[1] // DH
    carry = jnp.concatenate([carry_ref[:, h : h + 1] for h in range(heads)], axis=0)
    for step, block in enumerate(sent, 1):
        doc_row = block[rows : rows + 1, 0:rows].astype(jnp.float32)
        doc_row = jnp.where(place_ref[0] >= step, doc_row, -1.0)
        live = col_ref[...] == doc_row
        term, carry = block_terms(
            q_ref,
            bias_ref,
            lambda g, block=block: block[0:rows, g * DH : (g + 1) * DH],
            lambda g, block=block: block[0:rows, width + g * DH : width + (g + 1) * DH],
            live,
            carry,
        )
        mix = mix + term
    mixed_ref[...] = mix
    share = rows // len(order)
    for mask, out in zip(order, outs):
        first = pl.multiple_of((place_ref[1] ^ mask) * share, share)
        piece = mixed_ref[pl.ds(first, share), :].astype(jnp.bfloat16)
        out[...] = jnp.dot(piece, w_ref[...], preferred_element_type=jnp.float32).astype(jnp.bfloat16)


def norm_kernel(resid_ref, gain_ref, *refs):
    pieces, middle_ref, normed_ref = refs[:-2], refs[-2], refs[-1]
    total = pieces[0][...].astype(jnp.float32)
    for piece in pieces[1:]:
        total = total + piece[...].astype(jnp.float32)
    middle = (resid_ref[...].astype(jnp.float32) + total).astype(jnp.bfloat16)
    middle_ref[...] = middle
    value = middle.astype(jnp.float32)
    scale = lax.rsqrt(jnp.mean(value * value, axis=1, keepdims=True) + 1e-06)
    normed_ref[...] = (value * scale * gain_ref[...]).astype(jnp.bfloat16)


def expert_kernel(near_ref, far_ref, gate_ref, up_ref, down_ref, kept_ref, sent_ref, held_ref, hidden_ref):
    half = near_ref.shape[0]
    held_ref[:half, :] = near_ref[...]
    held_ref[half:, :] = far_ref[...]
    tile = 256
    for at in range(0, gate_ref.shape[2], tile):
        gate_value = jnp.dot(
            held_ref[...], gate_ref[0, :, at : at + tile], preferred_element_type=jnp.float32
        )
        up_value = jnp.dot(
            held_ref[...], up_ref[0, :, at : at + tile], preferred_element_type=jnp.float32
        )
        hidden = gate_value / (1.0 + jnp.exp(-gate_value)) * up_value
        hidden_ref[:, at : at + tile] = hidden.astype(jnp.bfloat16)
    for at in range(0, down_ref.shape[2], tile):
        result = jnp.dot(
            hidden_ref[...], down_ref[0, :, at : at + tile], preferred_element_type=jnp.float32
        ).astype(jnp.bfloat16)
        kept_ref[:, at : at + tile] = result[:half]
        sent_ref[:, at : at + tile] = result[half:]


def cost(flops, nbytes):
    return pl.CostEstimate(flops=flops, bytes_accessed=nbytes, transcendentals=0)


def middle_direct(queries, keys, values, head_bias, documents, w_out, resid, norm_gain):
    rows, width = queries.shape
    kv_width = keys.shape[1]
    sp_count = lax.axis_size("sp")
    tp_count = lax.axis_size("tp")
    doc_real = documents.astype(jnp.bfloat16)
    doc_rows = jnp.zeros((DOC_ROWS, 2 * kv_width), jnp.bfloat16)
    doc_rows = doc_rows.at[0, :rows].set(doc_real)
    packed = jnp.concatenate([jnp.concatenate([keys, values], axis=1), doc_rows], axis=0)
    sent = [shifted(packed, steps, False) for steps in range(1, sp_count)]
    col = documents.astype(jnp.float32).reshape(rows, 1)
    row = documents.astype(jnp.float32).reshape(1, rows)
    mix, carry = pl.pallas_call(
        here_kernel,
        out_shape=(
            jax.ShapeDtypeStruct((rows, width), jnp.float32),
            jax.ShapeDtypeStruct((rows, DH), jnp.float32),
        ),
        in_specs=[VMEM, VMEM, VMEM, SMEM, VMEM, VMEM],
        out_specs=(VMEM, VMEM),
        cost_estimate=cost(6 * 10**9, 10**6),
        name="attend_here",
    )(queries, keys, values, head_bias, col, row)
    place = jnp.stack([lax.axis_index("sp"), lax.axis_index("tp")]).astype(jnp.int32)
    order = list(range(tp_count))
    share = rows // tp_count
    pieces = pl.pallas_call(
        functools.partial(away_kernel, sp_count - 1, order),
        out_shape=[jax.ShapeDtypeStruct((share, D), jnp.bfloat16)] * tp_count,
        in_specs=[SMEM, VMEM, SMEM, VMEM, VMEM, VMEM, VMEM] + [VMEM] * (sp_count - 1),
        out_specs=[VMEM] * tp_count,
        scratch_shapes=[pltpu.VMEM((rows, width), jnp.float32)],
        cost_estimate=cost(10 * 10**9, 4 * 10**6),
        compiler_params=pltpu.CompilerParams(vmem_limit_bytes=SMALL),
        name="attend_away",
    )(place, queries, head_bias, col, mix, carry, w_out, *sent)
    arrived = [pieces[0]] + [swapped(pieces[mask], mask) for mask in order[:0:-1]]
    return pl.pallas_call(
        norm_kernel,
        out_shape=[jax.ShapeDtypeStruct((share, D), jnp.bfloat16)] * 2,
        in_specs=[VMEM] * (2 + tp_count),
        out_specs=[VMEM] * 2,
        cost_estimate=cost(10**8, 10**6),
        compiler_params=pltpu.CompilerParams(vmem_limit_bytes=SMALL),
        name="middle_norm",
    )(resid, norm_gain.reshape(1, D), *arrived)


def experts_dense(middle, normed, expert_ids, expert_gates, w_gate, w_up, w_down):
    rows = normed.shape[0]
    sp_count = lax.axis_size("sp")
    tp_count = lax.axis_size("tp")
    masks = [1 << bit for bit in range(tp_count.bit_length() - 1)]
    steps = [0] + [s for pair in zip(range(1, sp_count), range(sp_count - 1, 0, -1)) for s in pair]
    steps = list(dict.fromkeys(steps))
    chunks = [steps[:1]] + [steps[at : at + 2] for at in range(1, len(steps), 2)]
    moved = {0: normed}
    for chunk in chunks[1:]:
        for s in chunk:
            moved[s] = shifted(normed, s, True)
    pieces = {}
    for at, chunk in enumerate(chunks):
        held = jnp.concatenate([moved[s] for s in chunk], axis=0)
        for mask in masks[:0:-1]:
            other = swapped(held, mask)
            held = jnp.concatenate([held, other], axis=0)
        far = swapped(held, 1)
        count = held.shape[0]
        result, leaving = pl.pallas_call(
            expert_kernel,
            out_shape=[jax.ShapeDtypeStruct((count, D), jnp.bfloat16)] * 2,
            in_specs=[VMEM] * 5,
            out_specs=[VMEM] * 2,
            scratch_shapes=[
                pltpu.VMEM((2 * count, D), jnp.bfloat16),
                pltpu.VMEM((2 * count, w_gate.shape[2]), jnp.bfloat16),
            ],
            compiler_params=pltpu.CompilerParams(vmem_limit_bytes=32 * 2**20),
            cost_estimate=cost(12 * count * D * w_gate.shape[2], 12 * 10**6),
        )(held, far, w_gate, w_up, w_down)
        for mask in masks:
            if mask > 1:
                kept = result.shape[0] // 2
                result, leaving = result[:kept], result[kept:]
            other = swapped(leaving, mask)
            result = (result.astype(jnp.float32) + other.astype(jnp.float32)).astype(jnp.bfloat16)
        for at, s in enumerate(chunk):
            pieces[s] = result[at * rows : (at + 1) * rows]
    own = lax.axis_index("sp")
    total = middle.astype(jnp.float32)
    combined = jnp.zeros_like(total)
    for s in steps:
        piece = pieces[s] if s == 0 else shifted(pieces[s], -s, True)
        chosen = expert_ids == (own + s) % sp_count
        scale = jnp.sum(jnp.where(chosen, expert_gates, 0.0), axis=1, keepdims=True)
        combined = combined + scale * piece.astype(jnp.float32)
    return (total + combined).astype(jnp.bfloat16)


def passed_along(value, axis, steps):
    count = lax.axis_size(axis)
    initial, last = (max(0, -steps), min(count, count - steps))
    return lax.ppermute(value, axis, [(source, source + steps) for source in range(initial, last)])


def attend_terms(query_grid, bias_grid, key_block, value_block, live, carried):
    kv_local = bias_grid.shape[0]
    key_count = key_block.shape[0]
    logits = (
        jnp.einsum(
            "qgrd,sgd->grqs",
            query_grid,
            key_block.reshape(key_count, kv_local, DH),
            preferred_element_type=jnp.float32,
        )
        * DH ** (-0.5)
        + bias_grid[:, :, None, None]
    )
    keep = jnp.where(live, jax.nn.log_sigmoid(-logits), 0.0)
    after = lax.cumsum(keep, axis=3, reverse=True) - keep + carried[:, :, :, None]
    weight = jnp.where(live, jnp.exp(jax.nn.log_sigmoid(logits) + after), 0.0).astype(jnp.bfloat16)
    partial_mix = jnp.einsum(
        "grqs,sgd->qgrd",
        weight,
        value_block.reshape(key_count, kv_local, DH),
        preferred_element_type=jnp.float32,
    )
    return (partial_mix, jnp.sum(keep, axis=3))


def middle_ring(queries, keys, values, head_bias, documents, w_out, resid, norm_gain):
    tok_count = queries.shape[0]
    kv_local = keys.shape[1] // DH
    group_size = HEADS // KV_HEADS
    sp_count = lax.axis_size("sp")
    sp_index = lax.axis_index("sp")
    query_grid = queries.reshape(tok_count, kv_local, group_size, DH)
    bias_grid = head_bias.reshape(kv_local, group_size)
    doc_here = documents.astype(jnp.bfloat16)
    doc_column = doc_here.reshape(tok_count, 1)
    local_pos = jnp.arange(tok_count, dtype=jnp.int32)
    live_local = (local_pos[None, :] < local_pos[:, None]) & (
        documents[None, :] == documents[:, None]
    )
    zero_carry = jnp.zeros((kv_local, group_size, tok_count), jnp.float32)
    mix_total, carried = attend_terms(query_grid, bias_grid, keys, values, live_local, zero_carry)

    def visit(turn_index, state):
        mix_sum, carry_sum, key_block, value_block, doc_block = state
        key_block, value_block, doc_block = passed_along(
            (key_block, value_block, doc_block), "sp", 1
        )
        live = (doc_block[:, 0][None, :] == doc_here[:, None]) & (sp_index - turn_index >= 0)
        partial_mix, block_keep = attend_terms(
            query_grid, bias_grid, key_block, value_block, live, carry_sum
        )
        return (mix_sum + partial_mix, carry_sum + block_keep, key_block, value_block, doc_block)

    mix_total, carried, _, _, _ = lax.fori_loop(
        1, sp_count, visit, (mix_total, carried, keys, values, doc_column)
    )
    mixed = mix_total.reshape(tok_count, kv_local * group_size * DH).astype(jnp.bfloat16)
    projected = lax.psum_scatter(
        jnp.dot(mixed, w_out, preferred_element_type=jnp.float32).astype(jnp.bfloat16),
        "tp",
        scatter_dimension=0,
        tiled=True,
    ).astype(jnp.float32)
    middle = (resid.astype(jnp.float32) + projected).astype(jnp.bfloat16)
    middle_value = middle.astype(jnp.float32)
    normed = (
        middle_value
        * lax.rsqrt(jnp.mean(middle_value * middle_value, axis=1, keepdims=True) + 1e-06)
        * norm_gain
    ).astype(jnp.bfloat16)
    return middle, normed


def experts_routed(middle, normed, expert_ids, expert_gates, w_gate, w_up, w_down, slot_limit):
    middle_value = middle.astype(jnp.float32)
    sp_count = lax.axis_size("sp")
    tp_count = lax.axis_size("tp")
    row_count = normed.shape[0]
    expert_count = w_gate.shape[0] * sp_count
    flat_ids = expert_ids.reshape(-1)
    onehot_ids = (flat_ids[:, None] == jnp.arange(expert_count, dtype=jnp.int32)[None, :]).astype(
        jnp.int32
    )
    earlier = jnp.cumsum(onehot_ids, axis=0) - onehot_ids
    slot_ids = jnp.sum(earlier * onehot_ids, axis=1)
    target = flat_ids * slot_limit + slot_ids
    placing = (
        jnp.arange(expert_count * slot_limit, dtype=jnp.int32)[:, None] == target[None, :]
    ).astype(jnp.bfloat16)
    by_token = jnp.sum(placing.reshape(expert_count * slot_limit, row_count, TOPK), axis=2)
    outgoing = jnp.dot(by_token, normed, preferred_element_type=jnp.float32).astype(jnp.bfloat16)
    outgoing = outgoing.reshape(expert_count, slot_limit, D)
    arrived = lax.all_to_all(outgoing, "sp", split_axis=0, concat_axis=0, tiled=True)
    gathered = lax.all_gather(arrived, "tp", axis=0, tiled=True)
    expert_rows = gathered.reshape(-1, D)
    gate_value = jnp.dot(expert_rows, w_gate[0], preferred_element_type=jnp.float32)
    up_value = jnp.dot(expert_rows, w_up[0], preferred_element_type=jnp.float32)
    hidden = (jax.nn.silu(gate_value) * up_value).astype(jnp.bfloat16)
    partial_out = jnp.dot(hidden, w_down[0], preferred_element_type=jnp.float32)
    summed = lax.psum_scatter(
        partial_out.reshape(tp_count, sp_count * slot_limit, D).astype(jnp.bfloat16),
        "tp",
        scatter_dimension=0,
        tiled=True,
    ).astype(jnp.float32)
    expert_result = summed.reshape(sp_count, slot_limit, D).astype(jnp.bfloat16)
    returned = lax.all_to_all(expert_result, "sp", split_axis=0, concat_axis=0, tiled=True)
    routed = jnp.dot(placing.T, returned.reshape(-1, D), preferred_element_type=jnp.float32)
    combined = jnp.sum(expert_gates[:, :, None] * routed.reshape(row_count, TOPK, D), axis=1)
    return (middle_value + combined).astype(jnp.bfloat16)


def local(
    queries,
    keys,
    values,
    head_bias,
    documents,
    w_out,
    resid,
    norm_gain,
    expert_ids,
    expert_gates,
    w_gate,
    w_up,
    w_down,
):
    sp_count = lax.axis_size("sp")
    tp_count = lax.axis_size("tp")
    paired = tp_count & (tp_count - 1) == 0
    direct = paired and sp_count * keys.shape[0] <= DIRECT_KEYS and sp_count > 1
    middle_of = middle_direct if direct else middle_ring
    middle, normed = middle_of(
        queries, keys, values, head_bias, documents, w_out, resid, norm_gain
    )
    row_count = normed.shape[0]
    expert_count = w_gate.shape[0] * sp_count
    slot_limit = min(row_count, max(2, 2 * TOPK * row_count // expert_count))
    routing = (middle, normed, expert_ids, expert_gates, w_gate, w_up, w_down)
    if paired and slot_limit == row_count and w_gate.shape[0] == 1 and sp_count > 1:
        return experts_dense(*routing)
    return experts_routed(*routing, slot_limit)


def solution(mesh):
    return jax.shard_map(
        local,
        mesh=mesh,
        in_specs=(
            P(("grp", "sp"), "tp"),
            P(("grp", "sp"), "tp"),
            P(("grp", "sp"), "tp"),
            P("tp"),
            P(("grp", "sp")),
            P("tp", None),
            P(("grp", "sp", "tp"), None),
            P(),
            P(("grp", "sp", "tp"), None),
            P(("grp", "sp", "tp"), None),
            P("sp", None, "tp"),
            P("sp", None, "tp"),
            P("sp", "tp", None),
        ),
        out_specs=P(("grp", "sp", "tp"), None),
        check_vma=False,
    )
```
